256 devices in a mesh: grp: 2 (over y), sp: 16 (over z), tp: 8 (over x, core).
Axes of the slice: x: 4, y: 2, z: 16, core: 2. Of those that a mesh axis runs over, the one named last changes fastest.
The devices are a block of a 4x16x16 slice.
Arguments:
- source: bfloat16 [16384, 2048], P(('grp', 'sp', 'tp')), parts along dimension 0, may hold values from -8 to 8
- target: bfloat16 [4096, 2048], P(('grp', 'sp', 'tp')), parts along dimension 0, may hold values from -8 to 8
- source_gain: float32 [2048], replicated, may hold values from 0.1 to 1.9
- attend_gain: float32 [2, 2048], replicated, may hold values from 0.1 to 1.9
- query_weight: bfloat16 [2, 2048, 2048], P(None, None, 'tp'), may hold values from -4 to 4
- key_weight: bfloat16 [2, 2048, 2048], P(None, None, 'tp'), may hold values from -4 to 4
- value_weight: bfloat16 [2, 2048, 2048], P(None, None, 'tp'), may hold values from -0.125 to 0.125
- out_weight: bfloat16 [2, 2048, 2048], P(None, 'tp'), may hold values from -3 to 3
- mixer_gain: float32 [2048], replicated, may hold values from 0.1 to 1.9
- gate_weight: bfloat16 [2048, 2816], P(None, 'tp'), may hold values from -0.125 to 0.125
- up_weight: bfloat16 [2048, 2816], P(None, 'tp'), may hold values from -0.125 to 0.125
- gate_taps: float32 [3, 2816], P(None, 'tp'), may hold values from -3 to 3
- up_taps: float32 [3, 2816], P(None, 'tp'), may hold values from -3 to 3
- down_weight: bfloat16 [2816, 2048], P('tp'), may hold values from -0.109375 to 0.109375
- final_gain: float32 [2048], replicated, may hold values from 0.1 to 1.9
Outputs:
- result: bfloat16 [4096, 2048], P(('grp', 'sp', 'tp')), parts along dimension 0
The draws below stay inside these ranges and needn't reach their ends.
There are 2 independent parts, one for each index of `grp`. The reference program is written for one: setup_inputs(seed, part) draws one part's arguments, and reference() takes and returns one part's arrays. A program takes and returns all parts, laid end to end along the dimension named above; an argument that names none is the same for every part. Nothing has to cross between parts.
All inputs are finite; a program needn't handle non-finite values.
Results may differ from the reference program's by a relative error of at most 0.04.
Values may be sent and summed in bfloat16 or wider, within the bound.
No kernel may reach another device: no remote copies, remote signals or barrier semaphores. Data moves between devices by JAX's collectives and lax.ppermute only.
A program may use at most 128 MiB of HBM per device.

```python
import jax
import jax.numpy as jnp
from jax import lax

D = 2048
HEADS = 8
FF = 2816
HD = 256
SRC = 8192
TGT = 2048


def projection_draw(key, salt_value):
    stacked = []
    for layer_number in range(2):
        base_draw = jax.random.normal(jax.random.fold_in(key, salt_value * 10 + layer_number), (D, D), jnp.float32)
        layer_matrix = jnp.clip(base_draw, -6.0, 6.0) * D ** (-0.5)
        stacked.append(jnp.clip(layer_matrix, -4.0, 4.0))
    return jnp.stack(stacked).astype(jnp.bfloat16)


def row_draw(key, row_count):
    base_rows = jnp.clip(jax.random.normal(jax.random.fold_in(key, 1), (row_count, D), jnp.float32), -6.0, 6.0)
    return base_rows.astype(jnp.bfloat16)


def draw_source(key, part):
    return row_draw(key, SRC)


def draw_target(key, part):
    return row_draw(key, TGT)


def draw_query_weight(key, part):
    return projection_draw(key, 1)


def draw_key_weight(key, part):
    return projection_draw(key, 2)


def steps_of(own_key, shape, pieces, low, largest):
    level = 1.0
    for position, shards_of in pieces:
        draws = jax.random.uniform(jax.random.fold_in(jax.random.fold_in(own_key, 6), position), (shards_of,), jnp.float32, low / len(pieces), largest / len(pieces))
        level = level * jnp.repeat(jnp.exp(draws), shape[position] // shards_of).reshape((-1,) + (1,) * (len(shape) - 1 - position))
    return level


def centred(rng, extent, width, limit, split=(), kind=jnp.bfloat16):
    level = steps_of(rng, extent, split, -0.22, 0.18) if split else 1.0
    entries = jax.random.normal(rng, extent, jnp.float32) * width * level
    return jnp.minimum(jnp.maximum(entries, -limit), limit).astype(kind)


def setup_inputs(seed: int = 0, part: int = 0) -> dict:
    keys = jax.random.split(jax.random.key(seed), 16)
    own_keys = jax.random.split(jax.random.fold_in(keys[15], part), 16)
    return {
        "source": draw_source(jax.random.fold_in(jax.random.fold_in(keys[15], part), 71), part),
        "target": draw_target(jax.random.fold_in(jax.random.fold_in(keys[15], part), 71), part),
        "source_gain": jnp.clip(1.0 + 0.18 * jax.random.normal(keys[2], (D,), jnp.float32), 0.1, 1.9),
        "attend_gain": jnp.clip(1.0 + 0.18 * jax.random.normal(keys[3], (2, D), jnp.float32), 0.1, 1.9),
        "query_weight": draw_query_weight(jax.random.fold_in(keys[15], 71), part),
        "key_weight": draw_key_weight(jax.random.fold_in(keys[15], 71), part),
        "value_weight": centred(keys[6], (2, D, D), D ** -0.5, 0.125, ((2, 8),)),
        "out_weight": centred(keys[7], (2, D, D), 4 ** -0.5, 3.0, ((1, 8),)),
        "mixer_gain": jnp.clip(1.0 + 0.18 * jax.random.normal(keys[8], (D,), jnp.float32), 0.1, 1.9),
        "gate_weight": centred(keys[9], (D, FF), D ** -0.5, 0.125, ((1, 8),)),
        "up_weight": centred(keys[10], (D, FF), D ** -0.5, 0.125, ((1, 8),)),
        "gate_taps": centred(keys[11], (3, FF), 0.6, 3.0, ((1, 8),), jnp.float32),
        "up_taps": centred(keys[12], (3, FF), 0.6, 3.0, ((1, 8),), jnp.float32),
        "down_weight": centred(keys[13], (FF, D), FF ** -0.5, 0.109375, ((0, 8),)),
        "final_gain": jnp.clip(1.0 + 0.18 * jax.random.normal(keys[14], (D,), jnp.float32), 0.1, 1.9),
    }


EPS = 1e-06

def normed_rows(rows, gain):
    wide = rows.astype(jnp.float32)
    return wide * lax.rsqrt(lax.optimization_barrier(jnp.mean(wide * wide, axis=-1, keepdims=True)) + EPS) * gain

def one_head(triple):
    query_head, key_head, value_head = triple
    scores = jnp.dot(query_head, key_head.T, preferred_element_type=jnp.float32) * HD ** (-0.5)
    highest = lax.optimization_barrier(jnp.max(scores, axis=-1, keepdims=True))
    raised = jnp.exp(scores - highest)
    totals = lax.optimization_barrier(jnp.sum(raised, axis=-1, keepdims=True))
    weights = raised.astype(jnp.bfloat16)
    summed = jnp.dot(weights, value_head, preferred_element_type=jnp.float32)
    return (summed / totals).astype(jnp.bfloat16)

def split_heads(block):
    return block.reshape(block.shape[0], HEADS, HD).transpose(1, 0, 2)

def reference(source, target, source_gain, attend_gain, query_weight, key_weight, value_weight, out_weight, mixer_gain, gate_weight, up_weight, gate_taps, up_taps, down_weight, final_gain):
    source_normed = normed_rows(source, source_gain).astype(jnp.bfloat16)
    residual = target.astype(jnp.float32)
    for layer_number in range(2):
        normed = normed_rows(residual, attend_gain[layer_number]).astype(jnp.bfloat16)
        query_block = jnp.dot(normed, query_weight[layer_number], preferred_element_type=jnp.float32).astype(jnp.bfloat16)
        key_rows = jnp.dot(source_normed, key_weight[layer_number], preferred_element_type=jnp.float32).astype(jnp.bfloat16)
        value_rows = jnp.dot(source_normed, value_weight[layer_number], preferred_element_type=jnp.float32).astype(jnp.bfloat16)
        attended = lax.map(one_head, (split_heads(query_block), split_heads(key_rows), split_heads(value_rows)))
        attended = attended.transpose(1, 0, 2).reshape(query_block.shape[0], D)
        residual = residual + jnp.dot(attended, out_weight[layer_number], preferred_element_type=jnp.float32)
    mixed = normed_rows(residual, mixer_gain).astype(jnp.bfloat16)
    gated = jnp.dot(mixed, gate_weight, preferred_element_type=jnp.float32).astype(jnp.bfloat16)
    upped = jnp.dot(mixed, up_weight, preferred_element_type=jnp.float32).astype(jnp.bfloat16)
    zero_rows = jnp.zeros((2, FF), jnp.float32)
    gate_pad = jnp.concatenate([zero_rows, gated.astype(jnp.float32)], axis=0)
    up_pad = jnp.concatenate([zero_rows, upped.astype(jnp.float32)], axis=0)
    gate_conv = gate_taps[0] * gate_pad[:-2] + gate_taps[1] * gate_pad[1:-1] + gate_taps[2] * gate_pad[2:]
    up_conv = up_taps[0] * up_pad[:-2] + up_taps[1] * up_pad[1:-1] + up_taps[2] * up_pad[2:]
    hidden = (jax.nn.silu(gate_conv) * up_conv).astype(jnp.bfloat16)
    residual = residual + jnp.dot(hidden, down_weight, preferred_element_type=jnp.float32)
    return normed_rows(residual, final_gain).astype(jnp.bfloat16)
```

```python
import functools

import jax
import jax.numpy as jnp
from jax import lax
from jax.experimental import pallas as pl
from jax.experimental.pallas import tpu as pltpu
from jax.sharding import PartitionSpec as P

HD = 256
EPS = 1e-06
CORES = 2
SPAN = 4
STAT_ROWS = 8
HALO = 2
BF16 = jnp.bfloat16
F32 = jnp.float32


def core_swap(value):
    count = lax.axis_size("tp")
    return lax.ppermute(value, "tp", [(d, d ^ 1) for d in range(count)])


def chip_shift(value, steps):
    count = lax.axis_size("tp")
    return lax.ppermute(value, "tp", [(d, (d + CORES * steps) % count) for d in range(count)])


def block_shift(value, steps):
    count = lax.axis_size("sp")
    return lax.ppermute(value, "sp", [(d, (d + steps) % count) for d in range(count)])


def next_block(value):
    count = lax.axis_size("sp")
    return lax.ppermute(value, "sp", [(d, d + 1) for d in range(count - 1)])


def gathered(rows):
    chips = lax.axis_size("tp") // CORES
    near = jnp.concatenate([rows] + [chip_shift(rows, k) for k in range(1, chips)], axis=0)
    return jnp.concatenate([near, core_swap(near)], axis=0)


def summed_home(partial):
    chips = lax.axis_size("tp") // CORES
    half = partial.shape[0] // CORES
    rows = half // chips
    mine = partial[:half].astype(F32) + core_swap(partial[half:]).astype(F32)
    away = mine.astype(BF16)
    total = mine[:rows]
    for k in range(1, chips):
        total = total + chip_shift(away[k * rows : (k + 1) * rows], -k).astype(F32)
    return total


def normed_rows(rows, gain):
    wide = rows.astype(F32)
    return wide * lax.rsqrt(jnp.mean(wide * wide, axis=-1, keepdims=True) + EPS) * gain


def attend_kernel(*refs, pieces, blocks):
    query_refs = refs[:blocks]
    key_refs = refs[blocks : blocks + pieces]
    value_refs = refs[blocks + pieces : blocks + 2 * pieces]
    out_refs = refs[blocks + 2 * pieces : 2 * blocks + 2 * pieces]
    score_ref = refs[-1]
    count = query_refs[0].shape[0]
    for pair in range(blocks // 2):
        query = jnp.concatenate([query_refs[2 * pair][...], query_refs[2 * pair + 1][...]], axis=0)
        start = 0
        top = None
        for key_ref in key_refs:
            size = key_ref.shape[0]
            scores = lax.dot_general(
                key_ref[...], query, (((1,), (1,)), ((), ())), preferred_element_type=F32
            )
            score_ref[start : start + size, :] = scores
            highest = jnp.max(scores, axis=0, keepdims=True)
            top = highest if top is None else jnp.maximum(top, highest)
            start += size
        start = 0
        total = None
        summed = None
        for value_ref in value_refs:
            size = value_ref.shape[1]
            raised = jnp.exp(score_ref[start : start + size, :] - top)
            part_total = jnp.sum(raised, axis=0, keepdims=True)
            part = lax.dot_general(
                value_ref[...], raised.astype(BF16), (((1,), (0,)), ((), ())), preferred_element_type=F32
            )
            total = part_total if total is None else total + part_total
            summed = part if summed is None else summed + part
            start += size
        partial = (summed / total).astype(BF16)
        level = top + jnp.log(total)
        first = level.astype(BF16)
        rest = level - first.astype(F32)
        second = rest.astype(BF16)
        third = (rest - second.astype(F32)).astype(BF16)
        place = lax.broadcasted_iota(jnp.int32, (STAT_ROWS, 2 * count), 0)
        stats = jnp.where(
            place == 0,
            first.astype(F32),
            jnp.where(place == 1, second.astype(F32), jnp.where(place == 2, third.astype(F32), 0.0)),
        ).astype(BF16)
        for k in range(2):
            cut = slice(k * count, (k + 1) * count)
            out_refs[2 * pair + k][:HD, :] = partial[:, cut]
            out_refs[2 * pair + k][HD:, :] = stats[:, cut]


def attend(queries, keys, values):
    count = queries[0].shape[0]
    total = sum(k.shape[0] for k in keys)
    spec = pl.BlockSpec(memory_space=pltpu.VMEM)
    return pl.pallas_call(
        functools.partial(attend_kernel, pieces=len(keys), blocks=len(queries)),
        out_shape=[jax.ShapeDtypeStruct((HD + STAT_ROWS, count), BF16)] * len(queries),
        in_specs=[spec] * (len(queries) + len(keys) + len(values)),
        out_specs=[spec] * len(queries),
        scratch_shapes=[pltpu.VMEM((total, 2 * count), F32)],
        cost_estimate=pl.CostEstimate(
            flops=4 * total * count * len(queries) * HD,
            bytes_accessed=4 * total * HD,
            transcendentals=total * count * len(queries),
        ),
    )(*queries, *keys, *values)


def combine_kernel(*refs):
    parts, weight_ref, out_ref = refs[:-2], refs[-2], refs[-1]
    levels = []
    for part in parts:
        stats = part[HD:, :].astype(F32)
        levels.append(stats[0:1] + stats[1:2] + stats[2:3])
    top = functools.reduce(jnp.maximum, levels)
    shares = [jnp.exp(level - top) for level in levels]
    whole = functools.reduce(jnp.add, shares)
    summed = functools.reduce(
        jnp.add, [part[:HD, :].astype(F32) * (share / whole) for part, share in zip(parts, shares)]
    )
    out_ref[...] = lax.dot_general(
        summed.astype(BF16), weight_ref[...], (((0,), (0,)), ((), ())), preferred_element_type=F32
    ).astype(BF16)


def combined(parts, weight):
    spec = pl.BlockSpec(memory_space=pltpu.VMEM)
    return pl.pallas_call(
        combine_kernel,
        out_shape=jax.ShapeDtypeStruct((parts[0].shape[1], weight.shape[1]), BF16),
        in_specs=[spec] * (len(parts) + 1),
        out_specs=spec,
        cost_estimate=pl.CostEstimate(
            flops=2 * parts[0].shape[1] * weight.shape[0] * weight.shape[1],
            bytes_accessed=2 * weight.size,
            transcendentals=0,
        ),
    )(*parts, weight)


def dot(a, b):
    return jnp.dot(a, b, preferred_element_type=F32).astype(BF16)


def true_rows(count):
    device = lax.axis_index("tp")
    chips = lax.axis_size("tp") // CORES
    rows = count // (chips * CORES)
    i = lax.iota(jnp.int32, count)
    block, row = i // rows, i % rows
    core = (device % CORES) ^ (block // chips)
    chip = (device // CORES - block % chips + chips) % chips
    return (chip * CORES + core) * rows + row


def body(
    source,
    target,
    source_gain,
    attend_gain,
    query_weight,
    key_weight,
    value_weight,
    out_weight,
    mixer_gain,
    gate_weight,
    up_weight,
    gate_taps,
    up_taps,
    down_weight,
    final_gain,
):
    own = normed_rows(source, source_gain).astype(BF16)
    half = own.shape[0] // 2
    behind = block_shift(own, SPAN)
    ahead = block_shift(own, -SPAN)
    far = jnp.concatenate([block_shift(behind[:half], SPAN), block_shift(ahead[half:], -SPAN)], axis=0)
    pieces = [gathered(own), gathered(behind), gathered(ahead), gathered(far)]

    residual = target.astype(F32)
    for layer in range(2):
        keys = [dot(piece, key_weight[layer]) for piece in pieces]
        values = [
            lax.dot_general(
                value_weight[layer], piece, (((0,), (1,)), ((), ())), preferred_element_type=F32
            ).astype(BF16)
            for piece in pieces
        ]
        normed = normed_rows(residual, attend_gain[layer]).astype(BF16)
        query = dot(gathered(normed), query_weight[layer]) * BF16(HD**-0.5)
        offsets = (1, -1, -2)
        queries = [query] + [block_shift(query, k) for k in offsets]
        parts = attend(queries, keys, values)
        parts = [parts[0]] + [block_shift(part, -k) for part, k in zip(parts[1:], offsets)]
        residual = residual + summed_home(combined(parts, out_weight[layer]))

    mixed = gathered(normed_rows(residual, mixer_gain).astype(BF16))
    gated = dot(mixed, gate_weight)
    upped = dot(mixed, up_weight)
    lifted = jnp.concatenate([gated, upped], axis=1)
    count = lifted.shape[0]
    place = true_rows(count)
    pad = 8
    edge = lax.iota(jnp.int32, pad)
    pick = jnp.where(edge < HALO, count - HALO + edge, -1)
    last = jnp.dot((pick[:, None] == place[None, :]).astype(BF16), lifted, preferred_element_type=F32)
    earlier = next_block(last.astype(BF16))
    columns = jnp.concatenate([place, jnp.where(edge < HALO, edge - HALO, -count)])
    lifted = jnp.concatenate([lifted, earlier], axis=0)
    taps = jnp.concatenate([gate_taps, up_taps], axis=1)
    convolved = taps[2] * lifted[:count].astype(F32)
    for k in range(HALO):
        moved = ((place - HALO + k)[:, None] == columns[None, :]).astype(BF16)
        convolved = convolved + taps[k] * jnp.dot(moved, lifted, preferred_element_type=F32)
    inner = gate_weight.shape[1]
    hidden = (jax.nn.silu(convolved[:, :inner]) * convolved[:, inner:]).astype(BF16)
    residual = residual + summed_home(dot(hidden, down_weight))
    return normed_rows(residual, final_gain).astype(BF16)


def solution(mesh):
    placed = (
        P(("grp", "sp", "tp"), None),
        P(("grp", "sp", "tp"), None),
        P(),
        P(),
        P(None, None, "tp"),
        P(None, None, "tp"),
        P(None, None, "tp"),
        P(None, "tp", None),
        P(),
        P(None, "tp"),
        P(None, "tp"),
        P(None, "tp"),
        P(None, "tp"),
        P("tp", None),
        P(),
    )
    return jax.shard_map(
        body, mesh=mesh, in_specs=placed, out_specs=P(("grp", "sp", "tp"), None), check_vma=False
    )
```

```python
import functools

import jax
import jax.numpy as jnp
from jax import lax
from jax.experimental import pallas as pl
from jax.experimental.pallas import tpu as pltpu
from jax.sharding import Mesh
from jax.sharding import PartitionSpec as P


HD = 256
EPS = 1e-06
CORES = 2
TP = ("chip", "core")
SPAN = 4
STAT_ROWS = 8
HALO = 2
BF16 = jnp.bfloat16
F32 = jnp.float32


def core_swap(value):
    return lax.ppermute(value, "core", [(d, d ^ 1) for d in range(CORES)])


def chip_shift(value, steps):
    count = lax.axis_size("chip")
    return lax.ppermute(value, "chip", [(d, (d + steps) % count) for d in range(count)])


def block_shift(value, steps):
    count = lax.axis_size("sp")
    return lax.ppermute(value, "sp", [(d, (d + steps) % count) for d in range(count)])


def next_block(value):
    count = lax.axis_size("sp")
    return lax.ppermute(value, "sp", [(d, d + 1) for d in range(count - 1)])


def from_chips(rows):
    chips = lax.axis_size("chip")
    return jnp.concatenate([rows] + [chip_shift(rows, k) for k in range(1, chips)], axis=0)


def from_chips_both_ways(rows):
    half = rows.shape[0] // 2
    left = chip_shift(rows, 1)
    right = chip_shift(rows, -1)
    left_far = chip_shift(left[:half], 1)
    right_far = chip_shift(right[half:], -1)
    return jnp.concatenate([rows, left, left_far, right_far, right], axis=0)


def gathered(rows):
    near = from_chips(rows)
    return jnp.concatenate([near, core_swap(near)], axis=0)


def summed_home(mine, other):
    chips = lax.axis_size("chip")
    rows = mine.shape[0] // chips
    mine = mine.astype(F32) + core_swap(other).astype(F32)
    away = mine.astype(BF16)
    total = mine[:rows]
    for k in range(1, chips):
        total = total + chip_shift(away[k * rows : (k + 1) * rows], -k).astype(F32)
    return total


def normed_rows(rows, gain):
    wide = rows.astype(F32)
    return wide * lax.rsqrt(jnp.mean(wide * wide, axis=-1, keepdims=True) + EPS) * gain


def project_kernel(
    near_ref, other_ref, key_weight_ref, value_weight_ref, key_ref, value_ref, rows_ref, *, layer
):
    rows = near_ref.shape[0]
    step = 256
    rows_ref[:rows, :] = near_ref[...]
    rows_ref[rows:, :] = other_ref[...]

    def chunk(i, _):
        here = pl.ds(pl.multiple_of(i * step, step), step)
        block = rows_ref[here, :]
        key_ref[here, :] = jnp.dot(block, key_weight_ref[layer], preferred_element_type=F32).astype(BF16)
        values = jnp.dot(block, value_weight_ref[layer], preferred_element_type=F32)
        value_ref[:, here] = values.T.astype(BF16)
        return 0

    lax.fori_loop(0, 2 * rows // step, chunk, 0)


def project(piece, key_weight, value_weight, layer):
    near, other = piece
    rows = 2 * near.shape[0]
    spec = pl.BlockSpec(memory_space=pltpu.VMEM)
    return pl.pallas_call(
        functools.partial(project_kernel, layer=layer),
        out_shape=[jax.ShapeDtypeStruct((rows, HD), BF16), jax.ShapeDtypeStruct((HD, rows), BF16)],
        in_specs=[spec] * 4,
        out_specs=[spec] * 2,
        scratch_shapes=[pltpu.VMEM((rows, near.shape[1]), BF16)],
        compiler_params=pltpu.CompilerParams(vmem_limit_bytes=(6 << 20) + 14 * near.size),
        cost_estimate=pl.CostEstimate(
            flops=4 * rows * near.shape[1] * HD, bytes_accessed=2 * near.size, transcendentals=0
        ),
    )(near, other, key_weight, value_weight)


def attend_kernel(*refs, pieces, blocks):
    query_refs = refs[:blocks]
    key_refs = refs[blocks : blocks + pieces]
    value_refs = refs[blocks + pieces : blocks + 2 * pieces]
    out_refs = refs[blocks + 2 * pieces : 2 * blocks + 2 * pieces]
    query_all, key_all, value_all, score_ref, summed_ref, out_all = refs[-6:]
    count = query_refs[0].shape[0]
    for k, query_ref in enumerate(query_refs):
        query_all[k * count : (k + 1) * count, :] = query_ref[...]
    start = 0
    for key_ref, value_ref in zip(key_refs, value_refs):
        size = key_ref.shape[0]
        key_all[start : start + size, :] = key_ref[...]
        value_all[:, start : start + size] = value_ref[...]
        start += size
    step = 512
    steps = start // step

    def pair_step(pair, _):
        query = query_all[pl.ds(pl.multiple_of(pair * 2 * count, 2 * count), 2 * count), :]

        def score_step(i, top):
            here = pl.ds(pl.multiple_of(i * step, step), step)
            scores = lax.dot_general(
                key_all[here, :], query, (((1,), (1,)), ((), ())), preferred_element_type=F32
            )
            score_ref[here, :] = scores
            return jnp.maximum(top, jnp.max(scores, axis=0, keepdims=True))

        top = lax.fori_loop(0, steps, score_step, jnp.full((1, 2 * count), -jnp.inf, F32))
        summed_ref[...] = jnp.zeros_like(summed_ref)

        def sum_step(i, total):
            here = pl.ds(pl.multiple_of(i * step, step), step)
            raised = jnp.exp(score_ref[here, :] - top)
            summed_ref[...] += jnp.dot(
                value_all[:, here], raised.astype(BF16), preferred_element_type=F32
            )
            return total + jnp.sum(raised, axis=0, keepdims=True)

        total = lax.fori_loop(0, steps, sum_step, jnp.zeros((1, 2 * count), F32))
        summed = summed_ref[...]
        partial = (summed / total).astype(BF16)
        level = top + jnp.log(total)
        first = level.astype(BF16)
        rest = level - first.astype(F32)
        second = rest.astype(BF16)
        third = (rest - second.astype(F32)).astype(BF16)
        place = lax.broadcasted_iota(jnp.int32, (STAT_ROWS, 2 * count), 0)
        stats = jnp.where(
            place == 0,
            first.astype(F32),
            jnp.where(place == 1, second.astype(F32), jnp.where(place == 2, third.astype(F32), 0.0)),
        ).astype(BF16)
        out_all[pair, :HD, :] = partial
        out_all[pair, HD:, :] = stats
        return 0

    lax.fori_loop(0, blocks // 2, pair_step, 0)
    for k, out_ref in enumerate(out_refs):
        out_ref[...] = out_all[k // 2, :, (k % 2) * count : (k % 2 + 1) * count]


def attend(queries, keys, values):
    count = queries[0].shape[0]
    blocks = len(queries)
    total = sum(k.shape[0] for k in keys)
    spec = pl.BlockSpec(memory_space=pltpu.VMEM)
    return pl.pallas_call(
        functools.partial(attend_kernel, pieces=len(keys), blocks=blocks),
        out_shape=[jax.ShapeDtypeStruct((HD + STAT_ROWS, count), BF16)] * blocks,
        in_specs=[spec] * (blocks + len(keys) + len(values)),
        out_specs=[spec] * blocks,
        scratch_shapes=[
            pltpu.VMEM((blocks * count, HD), BF16),
            pltpu.VMEM((total, HD), BF16),
            pltpu.VMEM((HD, total), BF16),
            pltpu.VMEM((total, 2 * count), F32),
            pltpu.VMEM((HD, 2 * count), F32),
            pltpu.VMEM((blocks // 2, HD + STAT_ROWS, 2 * count), BF16),
        ],
        compiler_params=pltpu.CompilerParams(vmem_limit_bytes=12 << 20),
        cost_estimate=pl.CostEstimate(
            flops=4 * total * count * blocks * HD,
            bytes_accessed=4 * total * HD,
            transcendentals=total * count * blocks,
        ),
    )(*queries, *keys, *values)


def combine_kernel(*refs, layer):
    parts, weight_hbm, mine_ref, other_ref, weight_ref, arrived = refs[:-5], *refs[-5:]
    fetch = pltpu.make_async_copy(weight_hbm.at[layer], weight_ref, arrived)
    fetch.start()
    levels = []
    for part in parts:
        stats = part[HD:, :].astype(F32)
        levels.append(stats[0:1] + stats[1:2] + stats[2:3])
    top = functools.reduce(jnp.maximum, levels)
    shares = [jnp.exp(level - top) for level in levels]
    whole = functools.reduce(jnp.add, shares)
    summed = functools.reduce(
        jnp.add, [part[:HD, :].astype(F32) * (share / whole) for part, share in zip(parts, shares)]
    )
    attended = summed.T.astype(BF16)
    fetch.wait()
    half = mine_ref.shape[0]
    product = jnp.dot(attended, weight_ref[...], preferred_element_type=F32).astype(BF16)
    mine_ref[...] = product[:half]
    other_ref[...] = product[half:]


def combined(parts, weight, layer):
    spec = pl.BlockSpec(memory_space=pltpu.VMEM)
    count, width = parts[0].shape[1], weight.shape[2]
    half = jax.ShapeDtypeStruct((count // CORES, width), BF16)
    return pl.pallas_call(
        functools.partial(combine_kernel, layer=layer),
        out_shape=[half] * 2,
        in_specs=[spec] * len(parts) + [pl.BlockSpec(memory_space=pl.ANY)],
        out_specs=[spec] * 2,
        scratch_shapes=[pltpu.VMEM((HD, width), BF16), pltpu.SemaphoreType.DMA],
        compiler_params=pltpu.CompilerParams(vmem_limit_bytes=8 << 20),
        cost_estimate=pl.CostEstimate(
            flops=2 * count * HD * width, bytes_accessed=2 * HD * width, transcendentals=0
        ),
    )(*parts, weight)


def dot(a, b):
    return jnp.dot(a, b, preferred_element_type=F32).astype(BF16)


def true_rows(count):
    chips = lax.axis_size("chip")
    rows = count // (chips * CORES)
    i = lax.iota(jnp.int32, count)
    block, row = i // rows, i % rows
    core = lax.axis_index("core") ^ (block // chips)
    chip = (lax.axis_index("chip") - block % chips + chips) % chips
    return (chip * CORES + core) * rows + row


def whole(
    source,
    target,
    source_gain,
    attend_gain,
    query_weight,
    key_weight,
    value_weight,
    out_weight,
    mixer_gain,
    gate_weight,
    up_weight,
    gate_taps,
    up_taps,
    down_weight,
    final_gain,
):
    own = normed_rows(source, source_gain).astype(BF16)
    half = own.shape[0] // 2
    behind = block_shift(own, SPAN)
    ahead = block_shift(own, -SPAN)
    far = jnp.concatenate(
        [block_shift(behind[:half], SPAN), block_shift(ahead[half:], -SPAN)],
        axis=0,
    )
    slabs = {"own": own, "side": jnp.concatenate([behind, ahead], axis=0), "far": far}
    pieces = {}
    for name, slab in slabs.items():
        near = from_chips(slab) if name == "own" else from_chips_both_ways(slab)
        pieces[name] = (near, core_swap(near))

    residual = target.astype(F32)
    for layer in range(2):
        normed = normed_rows(residual, attend_gain[layer]).astype(BF16)
        rows = gathered(normed)
        query = dot(rows, query_weight[layer]) * BF16(HD**-0.5)
        projected = [project(piece, key_weight, value_weight, layer) for piece in pieces.values()]
        keys, values = zip(*projected)
        offsets = (1, -1, -2)
        queries = [query] + [block_shift(query, k) for k in offsets]
        parts = attend(queries, keys, values)
        parts = [parts[0]] + [block_shift(part, -k) for part, k in zip(parts[1:], offsets)]
        mine, other = combined(parts, out_weight, layer)
        residual = residual + summed_home(mine, other)

    mixed = gathered(normed_rows(residual, mixer_gain).astype(BF16))
    gated = dot(mixed, gate_weight)
    upped = dot(mixed, up_weight)
    lifted = jnp.concatenate([gated, upped], axis=1)
    count = lifted.shape[0]
    place = true_rows(count)
    pad = 8
    edge = lax.iota(jnp.int32, pad)
    pick = jnp.where(edge < HALO, count - HALO + edge, -1)
    last = jnp.dot((pick[:, None] == place[None, :]).astype(BF16), lifted, preferred_element_type=F32)
    earlier = next_block(last.astype(BF16))
    columns = jnp.concatenate([place, jnp.where(edge < HALO, edge - HALO, -count)])
    lifted = jnp.concatenate([lifted, earlier], axis=0)
    taps = jnp.concatenate([gate_taps, up_taps], axis=1)
    convolved = taps[2] * lifted[:count].astype(F32)
    for k in range(HALO):
        moved = ((place - HALO + k)[:, None] == columns[None, :]).astype(BF16)
        convolved = convolved + taps[k] * jnp.dot(moved, lifted, preferred_element_type=F32)
    inner = gate_weight.shape[1]
    hidden = (jax.nn.silu(convolved[:, :inner]) * convolved[:, inner:]).astype(BF16)
    product = dot(hidden, down_weight)
    half = product.shape[0] // CORES
    residual = residual + summed_home(product[:half], product[half:])
    return normed_rows(residual, final_gain).astype(BF16)


def solution(mesh):
    groups, blocks, _ = mesh.devices.shape
    mesh = Mesh(mesh.devices.reshape(groups, blocks, -1, CORES), ("grp", "sp", *TP))
    placed = (
        P(("grp", "sp", *TP), None),
        P(("grp", "sp", *TP), None),
        P(),
        P(),
        P(None, None, TP),
        P(None, None, TP),
        P(None, None, TP),
        P(None, TP, None),
        P(),
        P(None, TP),
        P(None, TP),
        P(None, TP),
        P(None, TP),
        P(TP, None),
        P(),
    )
    return jax.shard_map(
        whole, mesh=mesh, in_specs=placed, out_specs=P(("grp", "sp", *TP), None), check_vma=False
    )
```

```python
import functools

import jax
import jax.numpy as jnp
from jax import lax
from jax.experimental import pallas as pl
from jax.experimental.pallas import tpu as pltpu
from jax.sharding import Mesh
from jax.sharding import PartitionSpec as P


HD = 256
EPS = 1e-06
CORES = 2
TP = ("chip", "core")
SPAN = 4
STAT_ROWS = 8
HALO = 2
COPY_ROWS = 32
BF16 = jnp.bfloat16
F32 = jnp.float32


def core_swap(value):
    return lax.ppermute(value, "core", [(d, d ^ 1) for d in range(CORES)])


def chip_shift(value, steps):
    count = lax.axis_size("chip")
    return lax.ppermute(value, "chip", [(d, (d + steps) % count) for d in range(count)])


def block_shift(value, steps):
    count = lax.axis_size("sp")
    return lax.ppermute(value, "sp", [(d, (d + steps) % count) for d in range(count)])


def next_block(value):
    count = lax.axis_size("sp")
    return lax.ppermute(value, "sp", [(d, d + 1) for d in range(count - 1)])


def from_chips(rows):
    chips = lax.axis_size("chip")
    return jnp.concatenate([rows] + [chip_shift(rows, k) for k in range(1, chips)], axis=0)


def from_chips_both_ways(rows):
    half = rows.shape[0] // 2
    left = chip_shift(rows, 1)
    right = chip_shift(rows, -1)
    left_far = chip_shift(left[:half], 1)
    right_far = chip_shift(right[half:], -1)
    return jnp.concatenate([rows, left, left_far, right_far, right], axis=0)


def gathered_by_sends(rows):
    count = rows.shape[0]
    chips = lax.axis_size("chip")
    here = lax.axis_index("chip")
    near = jnp.zeros((chips * count, rows.shape[1]), rows.dtype)
    for k in range(chips):
        piece = chip_shift(rows, k) if k else rows
        near = lax.dynamic_update_slice(near, piece, ((here - k + chips) % chips * count, 0))
    return jnp.concatenate([near, core_swap(near)], axis=0)


def gathered(rows):
    chips = lax.axis_size("chip")
    copies = jnp.broadcast_to(rows[None], (chips, *rows.shape))
    near = lax.all_to_all(copies, "chip", 0, 0, tiled=True).reshape(-1, rows.shape[1])
    return jnp.concatenate([near, core_swap(near)], axis=0)


def summed_home(mine, other):
    chips = lax.axis_size("chip")
    rows = mine.shape[0] // chips
    mine = (mine.astype(F32) + core_swap(other).astype(F32)).astype(BF16)
    tiles = lax.all_to_all(mine.reshape(chips, rows, -1), "chip", 0, 0, tiled=True)
    return tiles.astype(F32).sum(axis=0)


def normed_rows(rows, gain):
    wide = rows.astype(F32)
    return wide * lax.rsqrt(jnp.mean(wide * wide, axis=-1, keepdims=True) + EPS) * gain


def project_kernel(*refs, layers):
    *halves, key_weight_ref, value_weight_ref, key_ref, value_ref, rows_ref = refs
    step = 256
    start = 0
    for ref in halves:

        def copy(i, _, start=start, ref=ref):
            here = pl.ds(pl.multiple_of(i * COPY_ROWS, COPY_ROWS), COPY_ROWS)
            there = pl.ds(pl.multiple_of(start + i * COPY_ROWS, COPY_ROWS), COPY_ROWS)
            rows_ref[there, :] = ref[here, :]
            return 0

        lax.fori_loop(0, ref.shape[0] // COPY_ROWS, copy, 0)
        start += ref.shape[0]
    steps = start // step

    def chunk(i, _):
        here = pl.ds(pl.multiple_of(i % steps * step, step), step)
        slot = i // steps
        layer = layers[0] + slot
        block = rows_ref[here, :]
        keys = jnp.dot(block, key_weight_ref[layer], preferred_element_type=F32)
        key_ref[slot, here, :] = keys.astype(BF16)
        values = jnp.dot(block, value_weight_ref[layer], preferred_element_type=F32)
        value_ref[slot, :, here] = values.T.astype(BF16)
        return 0

    lax.fori_loop(0, len(layers) * steps, chunk, 0)


def project(halves, key_weight, value_weight, layers):
    rows = sum(half.shape[0] for half in halves)
    width = halves[0].shape[1]
    spec = pl.BlockSpec(memory_space=pltpu.VMEM)
    return pl.pallas_call(
        functools.partial(project_kernel, layers=layers),
        out_shape=[
            jax.ShapeDtypeStruct((len(layers), rows, HD), BF16),
            jax.ShapeDtypeStruct((len(layers), HD, rows), BF16),
        ],
        in_specs=[spec] * (len(halves) + 2),
        out_specs=[spec] * 2,
        scratch_shapes=[pltpu.VMEM((rows, width), BF16)],
        compiler_params=pltpu.CompilerParams(vmem_limit_bytes=(6 << 20) + 7 * rows * width),
        cost_estimate=pl.CostEstimate(
            flops=4 * rows * width * HD * len(layers), bytes_accessed=2 * rows * width, transcendentals=0
        ),
    )(*halves, key_weight, value_weight)


def attend_kernel(*refs, pieces, blocks, slots):
    query_refs = refs[:blocks]
    key_refs = refs[blocks : blocks + pieces]
    value_refs = refs[blocks + pieces : blocks + 2 * pieces]
    out_refs = refs[blocks + 2 * pieces : 2 * blocks + 2 * pieces]
    query_all, key_all, value_all, score_ref, summed_ref, out_all = refs[-6:]
    count = query_refs[0].shape[0]
    for k, query_ref in enumerate(query_refs):
        query_all[k * count : (k + 1) * count, :] = query_ref[...]
    start = 0
    for key_ref, value_ref, slot in zip(key_refs, value_refs, slots):
        size = key_ref.shape[1]

        def copy_keys(i, _, start=start, key_ref=key_ref, slot=slot):
            here = pl.ds(pl.multiple_of(i * COPY_ROWS, COPY_ROWS), COPY_ROWS)
            there = pl.ds(pl.multiple_of(start + i * COPY_ROWS, COPY_ROWS), COPY_ROWS)
            key_all[there, :] = key_ref[slot, here, :]
            return 0

        def copy_values(i, _, start=start, size=size, value_ref=value_ref, slot=slot):
            here = pl.ds(pl.multiple_of(i * COPY_ROWS, COPY_ROWS), COPY_ROWS)
            value_all[here, start : start + size] = value_ref[slot, here, :]
            return 0

        lax.fori_loop(0, size // COPY_ROWS, copy_keys, 0)
        lax.fori_loop(0, HD // COPY_ROWS, copy_values, 0)
        start += size
    step = 512
    steps = start // step

    def pair_step(pair, _):
        query = query_all[pl.ds(pl.multiple_of(pair * 2 * count, 2 * count), 2 * count), :]

        def score_step(i, top):
            here = pl.ds(pl.multiple_of(i * step, step), step)
            scores = lax.dot_general(
                key_all[here, :], query, (((1,), (1,)), ((), ())), preferred_element_type=F32
            )
            score_ref[here, :] = scores
            return jnp.maximum(top, jnp.max(scores, axis=0, keepdims=True))

        top = lax.fori_loop(0, steps, score_step, jnp.full((1, 2 * count), -jnp.inf, F32))
        summed_ref[...] = jnp.zeros_like(summed_ref)

        def sum_step(i, total):
            here = pl.ds(pl.multiple_of(i * step, step), step)
            raised = jnp.exp(score_ref[here, :] - top)
            summed_ref[...] += jnp.dot(
                value_all[:, here], raised.astype(BF16), preferred_element_type=F32
            )
            return total + jnp.sum(raised, axis=0, keepdims=True)

        total = lax.fori_loop(0, steps, sum_step, jnp.zeros((1, 2 * count), F32))
        summed = summed_ref[...]
        partial = (summed / total).astype(BF16)
        level = top + jnp.log(total)
        first = level.astype(BF16)
        rest = level - first.astype(F32)
        second = rest.astype(BF16)
        third = (rest - second.astype(F32)).astype(BF16)
        place = lax.broadcasted_iota(jnp.int32, (STAT_ROWS, 2 * count), 0)
        stats = jnp.where(
            place == 0,
            first.astype(F32),
            jnp.where(place == 1, second.astype(F32), jnp.where(place == 2, third.astype(F32), 0.0)),
        ).astype(BF16)
        out_all[pair, :HD, :] = partial
        out_all[pair, HD:, :] = stats
        return 0

    lax.fori_loop(0, blocks // 2, pair_step, 0)
    for k, out_ref in enumerate(out_refs):
        out_ref[...] = out_all[k // 2, :, (k % 2) * count : (k % 2 + 1) * count]


def attend(queries, keys, values, slots):
    count = queries[0].shape[0]
    blocks = len(queries)
    total = sum(k.shape[1] for k in keys)
    spec = pl.BlockSpec(memory_space=pltpu.VMEM)
    return pl.pallas_call(
        functools.partial(attend_kernel, pieces=len(keys), blocks=blocks, slots=slots),
        out_shape=[jax.ShapeDtypeStruct((HD + STAT_ROWS, count), BF16)] * blocks,
        in_specs=[spec] * (blocks + len(keys) + len(values)),
        out_specs=[spec] * blocks,
        scratch_shapes=[
            pltpu.VMEM((blocks * count, HD), BF16),
            pltpu.VMEM((total, HD), BF16),
            pltpu.VMEM((HD, total), BF16),
            pltpu.VMEM((total, 2 * count), F32),
            pltpu.VMEM((HD, 2 * count), F32),
            pltpu.VMEM((blocks // 2, HD + STAT_ROWS, 2 * count), BF16),
        ],
        compiler_params=pltpu.CompilerParams(vmem_limit_bytes=12 << 20),
        cost_estimate=pl.CostEstimate(
            flops=4 * total * count * blocks * HD,
            bytes_accessed=4 * total * HD,
            transcendentals=total * count * blocks,
        ),
    )(*queries, *keys, *values)


def combine_kernel(*refs, layer):
    parts, weight_hbm, mine_ref, other_ref, weight_ref, arrived = refs[:-5], *refs[-5:]
    fetch = pltpu.make_async_copy(weight_hbm.at[layer], weight_ref, arrived)
    fetch.start()
    levels = []
    for part in parts:
        stats = part[HD:, :].astype(F32)
        levels.append(stats[0:1] + stats[1:2] + stats[2:3])
    top = functools.reduce(jnp.maximum, levels)
    shares = [jnp.exp(level - top) for level in levels]
    whole = functools.reduce(jnp.add, shares)
    summed = functools.reduce(
        jnp.add, [part[:HD, :].astype(F32) * (share / whole) for part, share in zip(parts, shares)]
    )
    attended = summed.T.astype(BF16)
    fetch.wait()
    half = mine_ref.shape[0]
    step = 512

    def columns(i, _):
        here = pl.ds(pl.multiple_of(i * step, step), step)
        product = jnp.dot(attended, weight_ref[:, here], preferred_element_type=F32).astype(BF16)
        mine_ref[:, here] = product[:half]
        other_ref[:, here] = product[half:]
        return 0

    lax.fori_loop(0, weight_ref.shape[1] // step, columns, 0)


def combined(parts, weight, layer):
    spec = pl.BlockSpec(memory_space=pltpu.VMEM)
    count, width = parts[0].shape[1], weight.shape[2]
    half = jax.ShapeDtypeStruct((count // CORES, width), BF16)
    return pl.pallas_call(
        functools.partial(combine_kernel, layer=layer),
        out_shape=[half] * 2,
        in_specs=[spec] * len(parts) + [pl.BlockSpec(memory_space=pl.ANY)],
        out_specs=[spec] * 2,
        scratch_shapes=[pltpu.VMEM((HD, width), BF16), pltpu.SemaphoreType.DMA],
        compiler_params=pltpu.CompilerParams(vmem_limit_bytes=8 << 20),
        cost_estimate=pl.CostEstimate(
            flops=2 * count * HD * width, bytes_accessed=2 * HD * width, transcendentals=0
        ),
    )(*parts, weight)


def dot(a, b):
    return jnp.dot(a, b, preferred_element_type=F32).astype(BF16)


def true_rows(count):
    chips = lax.axis_size("chip")
    rows = count // (chips * CORES)
    i = lax.iota(jnp.int32, count)
    block, row = i // rows, i % rows
    core = lax.axis_index("core") ^ (block // chips)
    return (block % chips * CORES + core) * rows + row


def whole(
    source,
    target,
    source_gain,
    attend_gain,
    query_weight,
    key_weight,
    value_weight,
    out_weight,
    mixer_gain,
    gate_weight,
    up_weight,
    gate_taps,
    up_taps,
    down_weight,
    final_gain,
):
    own = normed_rows(source, source_gain).astype(BF16)
    half = own.shape[0] // 2
    behind = block_shift(own, SPAN)
    ahead = block_shift(own, -SPAN)
    far = jnp.concatenate(
        [block_shift(behind[:half], SPAN), block_shift(ahead[half:], -SPAN)],
        axis=0,
    )
    slabs = {"own": own, "side": jnp.concatenate([behind, ahead], axis=0), "far": far}
    pieces = {}
    for name, slab in slabs.items():
        near = from_chips_both_ways(slab) if name == "side" else from_chips(slab)
        pieces[name] = (near, core_swap(near))

    residual = target.astype(F32)
    for layer in range(2):
        normed = normed_rows(residual, attend_gain[layer]).astype(BF16)
        rows = gathered(normed) if layer else gathered_by_sends(normed)
        query = dot(rows, query_weight[layer]) * BF16(HD**-0.5)
        if layer == 0:
            own_kv = project(pieces["own"], key_weight, value_weight, (0, 1))
            others = [
                project(pieces[name], key_weight, value_weight, (0,))
                for name in ("side", "far")
            ]
        else:
            others = [project(pieces["side"] + pieces["far"], key_weight, value_weight, (layer,))]
        keys, values = zip(own_kv, *others)
        slots = (layer,) + (0,) * len(others)
        offsets = (1, -1, -2)
        queries = [query] + [block_shift(query, k) for k in offsets]
        parts = attend(queries, keys, values, slots)
        parts = [parts[0]] + [block_shift(part, -k) for part, k in zip(parts[1:], offsets)]
        mine, other = combined(parts, out_weight, layer)
        residual = residual + summed_home(mine, other)

    mixed = gathered(normed_rows(residual, mixer_gain).astype(BF16))
    gated = dot(mixed, gate_weight)
    upped = dot(mixed, up_weight)
    lifted = jnp.concatenate([gated, upped], axis=1)
    count = lifted.shape[0]
    place = lax.optimization_barrier(true_rows(count))
    pad = 8
    edge = lax.iota(jnp.int32, pad)
    pick = jnp.where(edge < HALO, count - HALO + edge, -1)
    last = jnp.dot((pick[:, None] == place[None, :]).astype(BF16), lifted, preferred_element_type=F32)
    earlier = next_block(last.astype(BF16))
    columns = jnp.concatenate([place, jnp.where(edge < HALO, edge - HALO, -count)])
    lifted = jnp.concatenate([lifted, earlier], axis=0)
    taps = jnp.concatenate([gate_taps, up_taps], axis=1)
    convolved = taps[2] * lifted[:count].astype(F32)
    wanted = jnp.concatenate([place - HALO + k for k in range(HALO)])
    moved = jnp.dot(
        (wanted[:, None] == columns[None, :]).astype(BF16), lifted, preferred_element_type=F32
    )
    for k in range(HALO):
        convolved = convolved + taps[k] * moved[k * count : (k + 1) * count]
    inner = gate_weight.shape[1]
    hidden = (jax.nn.silu(convolved[:, :inner]) * convolved[:, inner:]).astype(BF16)
    product = dot(hidden, down_weight)
    half = product.shape[0] // CORES
    residual = residual + summed_home(product[:half], product[half:])
    return normed_rows(residual, final_gain).astype(BF16)


def solution(mesh):
    groups, blocks, _ = mesh.devices.shape
    mesh = Mesh(mesh.devices.reshape(groups, blocks, -1, CORES), ("grp", "sp", *TP))
    placed = (
        P(("grp", "sp", *TP), None),
        P(("grp", "sp", *TP), None),
        P(),
        P(),
        P(None, None, TP),
        P(None, None, TP),
        P(None, None, TP),
        P(None, TP, None),
        P(),
        P(None, TP),
        P(None, TP),
        P(None, TP),
        P(None, TP),
        P(TP, None),
        P(),
    )
    return jax.shard_map(
        whole, mesh=mesh, in_specs=placed, out_specs=P(("grp", "sp", *TP), None), check_vma=False
    )
```

```python
import functools

import jax
import jax.numpy as jnp
from jax import lax
from jax.experimental import pallas as pl
from jax.experimental.pallas import tpu as pltpu
from jax.sharding import Mesh
from jax.sharding import PartitionSpec as P


HD = 256
EPS = 1e-06
CORES = 2
TP = ("chip", "core")
SPAN = 4
STAT_ROWS = 8
HALO = 2
COPY_ROWS = 32
BF16 = jnp.bfloat16
F32 = jnp.float32


def core_swap(value):
    return lax.ppermute(value, "core", [(d, d ^ 1) for d in range(CORES)])


def chip_shift(value, steps):
    count = lax.axis_size("chip")
    return lax.ppermute(value, "chip", [(d, (d + steps) % count) for d in range(count)])


def block_shift(value, steps):
    count = lax.axis_size("sp")
    return lax.ppermute(value, "sp", [(d, (d + steps) % count) for d in range(count)])


def next_block(value):
    count = lax.axis_size("sp")
    return lax.ppermute(value, "sp", [(d, d + 1) for d in range(count - 1)])


def from_chips(rows):
    chips = lax.axis_size("chip")
    return jnp.concatenate([rows] + [chip_shift(rows, k) for k in range(1, chips)], axis=0)


def from_chips_both_ways(rows):
    half = rows.shape[0] // 2
    left = chip_shift(rows, 1)
    right = chip_shift(rows, -1)
    left_far = chip_shift(left[:half], 1)
    right_far = chip_shift(right[half:], -1)
    return jnp.concatenate([rows, left, left_far, right_far, right], axis=0)


def gathered(rows):
    near = from_chips(rows)
    return jnp.concatenate([near, core_swap(near)], axis=0)


def summed_home(mine, other):
    chips = lax.axis_size("chip")
    rows = mine.shape[0] // chips
    mine = mine.astype(F32) + core_swap(other).astype(F32)
    away = mine.astype(BF16)
    total = mine[:rows]
    for k in range(1, chips):
        total = total + chip_shift(away[k * rows : (k + 1) * rows], -k).astype(F32)
    return total


def normed_rows(rows, gain):
    wide = rows.astype(F32)
    return wide * lax.rsqrt(jnp.mean(wide * wide, axis=-1, keepdims=True) + EPS) * gain


def project_kernel(*refs, layers):
    *halves, key_weight_ref, value_weight_ref, key_ref, value_ref, rows_ref = refs
    step = 256
    start = 0
    for ref in halves:

        def copy(i, _, start=start, ref=ref):
            here = pl.ds(pl.multiple_of(i * COPY_ROWS, COPY_ROWS), COPY_ROWS)
            there = pl.ds(pl.multiple_of(start + i * COPY_ROWS, COPY_ROWS), COPY_ROWS)
            rows_ref[there, :] = ref[here, :]
            return 0

        lax.fori_loop(0, ref.shape[0] // COPY_ROWS, copy, 0)
        start += ref.shape[0]
    steps = start // step

    def chunk(i, _):
        here = pl.ds(pl.multiple_of(i % steps * step, step), step)
        slot = i // steps
        layer = layers[0] + slot
        block = rows_ref[here, :]
        keys = jnp.dot(block, key_weight_ref[layer], preferred_element_type=F32)
        key_ref[slot, here, :] = keys.astype(BF16)
        values = jnp.dot(block, value_weight_ref[layer], preferred_element_type=F32)
        value_ref[slot, :, here] = values.T.astype(BF16)
        return 0

    lax.fori_loop(0, len(layers) * steps, chunk, 0)


def project(halves, key_weight, value_weight, layers):
    rows = sum(half.shape[0] for half in halves)
    width = halves[0].shape[1]
    spec = pl.BlockSpec(memory_space=pltpu.VMEM)
    return pl.pallas_call(
        functools.partial(project_kernel, layers=layers),
        out_shape=[
            jax.ShapeDtypeStruct((len(layers), rows, HD), BF16),
            jax.ShapeDtypeStruct((len(layers), HD, rows), BF16),
        ],
        in_specs=[spec] * (len(halves) + 2),
        out_specs=[spec] * 2,
        scratch_shapes=[pltpu.VMEM((rows, width), BF16)],
        compiler_params=pltpu.CompilerParams(vmem_limit_bytes=(6 << 20) + 7 * rows * width),
        cost_estimate=pl.CostEstimate(
            flops=4 * rows * width * HD * len(layers), bytes_accessed=2 * rows * width, transcendentals=0
        ),
    )(*halves, key_weight, value_weight)


def attend_kernel(*refs, pieces, blocks, slots):
    query_refs = refs[:blocks]
    key_refs = refs[blocks : blocks + pieces]
    value_refs = refs[blocks + pieces : blocks + 2 * pieces]
    out_refs = refs[blocks + 2 * pieces : 2 * blocks + 2 * pieces]
    query_all, key_all, value_all, score_ref, summed_ref, out_all = refs[-6:]
    count = query_refs[0].shape[0]
    for k, query_ref in enumerate(query_refs):
        query_all[k * count : (k + 1) * count, :] = query_ref[...]
    start = 0
    for key_ref, value_ref, slot in zip(key_refs, value_refs, slots):
        size = key_ref.shape[1]

        def copy_keys(i, _, start=start, key_ref=key_ref, slot=slot):
            here = pl.ds(pl.multiple_of(i * COPY_ROWS, COPY_ROWS), COPY_ROWS)
            there = pl.ds(pl.multiple_of(start + i * COPY_ROWS, COPY_ROWS), COPY_ROWS)
            key_all[there, :] = key_ref[slot, here, :]
            return 0

        def copy_values(i, _, start=start, size=size, value_ref=value_ref, slot=slot):
            here = pl.ds(pl.multiple_of(i * COPY_ROWS, COPY_ROWS), COPY_ROWS)
            value_all[here, start : start + size] = value_ref[slot, here, :]
            return 0

        lax.fori_loop(0, size // COPY_ROWS, copy_keys, 0)
        lax.fori_loop(0, HD // COPY_ROWS, copy_values, 0)
        start += size
    step = 512
    steps = start // step

    def pair_step(pair, _):
        query = query_all[pl.ds(pl.multiple_of(pair * 2 * count, 2 * count), 2 * count), :]

        def score_step(i, top):
            here = pl.ds(pl.multiple_of(i * step, step), step)
            scores = lax.dot_general(
                key_all[here, :], query, (((1,), (1,)), ((), ())), preferred_element_type=F32
            )
            score_ref[here, :] = scores
            return jnp.maximum(top, jnp.max(scores, axis=0, keepdims=True))

        top = lax.fori_loop(0, steps, score_step, jnp.full((1, 2 * count), -jnp.inf, F32))
        summed_ref[...] = jnp.zeros_like(summed_ref)

        def sum_step(i, total):
            here = pl.ds(pl.multiple_of(i * step, step), step)
            raised = jnp.exp(score_ref[here, :] - top)
            summed_ref[...] += jnp.dot(
                value_all[:, here], raised.astype(BF16), preferred_element_type=F32
            )
            return total + jnp.sum(raised, axis=0, keepdims=True)

        total = lax.fori_loop(0, steps, sum_step, jnp.zeros((1, 2 * count), F32))
        summed = summed_ref[...]
        partial = (summed / total).astype(BF16)
        level = top + jnp.log(total)
        first = level.astype(BF16)
        rest = level - first.astype(F32)
        second = rest.astype(BF16)
        third = (rest - second.astype(F32)).astype(BF16)
        place = lax.broadcasted_iota(jnp.int32, (STAT_ROWS, 2 * count), 0)
        stats = jnp.where(
            place == 0,
            first.astype(F32),
            jnp.where(place == 1, second.astype(F32), jnp.where(place == 2, third.astype(F32), 0.0)),
        ).astype(BF16)
        out_all[pair, :HD, :] = partial
        out_all[pair, HD:, :] = stats
        return 0

    lax.fori_loop(0, blocks // 2, pair_step, 0)
    for k, out_ref in enumerate(out_refs):
        out_ref[...] = out_all[k // 2, :, (k % 2) * count : (k % 2 + 1) * count]


def attend(queries, keys, values, slots):
    count = queries[0].shape[0]
    blocks = len(queries)
    total = sum(k.shape[1] for k in keys)
    spec = pl.BlockSpec(memory_space=pltpu.VMEM)
    return pl.pallas_call(
        functools.partial(attend_kernel, pieces=len(keys), blocks=blocks, slots=slots),
        out_shape=[jax.ShapeDtypeStruct((HD + STAT_ROWS, count), BF16)] * blocks,
        in_specs=[spec] * (blocks + len(keys) + len(values)),
        out_specs=[spec] * blocks,
        scratch_shapes=[
            pltpu.VMEM((blocks * count, HD), BF16),
            pltpu.VMEM((total, HD), BF16),
            pltpu.VMEM((HD, total), BF16),
            pltpu.VMEM((total, 2 * count), F32),
            pltpu.VMEM((HD, 2 * count), F32),
            pltpu.VMEM((blocks // 2, HD + STAT_ROWS, 2 * count), BF16),
        ],
        compiler_params=pltpu.CompilerParams(vmem_limit_bytes=12 << 20),
        cost_estimate=pl.CostEstimate(
            flops=4 * total * count * blocks * HD,
            bytes_accessed=4 * total * HD,
            transcendentals=total * count * blocks,
        ),
    )(*queries, *keys, *values)


def combine_kernel(*refs, layer):
    parts, weight_hbm, mine_ref, other_ref, weight_ref, arrived = refs[:-5], *refs[-5:]
    fetch = pltpu.make_async_copy(weight_hbm.at[layer], weight_ref, arrived)
    fetch.start()
    levels = []
    for part in parts:
        stats = part[HD:, :].astype(F32)
        levels.append(stats[0:1] + stats[1:2] + stats[2:3])
    top = functools.reduce(jnp.maximum, levels)
    shares = [jnp.exp(level - top) for level in levels]
    whole = functools.reduce(jnp.add, shares)
    summed = functools.reduce(
        jnp.add, [part[:HD, :].astype(F32) * (share / whole) for part, share in zip(parts, shares)]
    )
    attended = summed.T.astype(BF16)
    fetch.wait()
    half = mine_ref.shape[0]
    product = jnp.dot(attended, weight_ref[...], preferred_element_type=F32).astype(BF16)
    mine_ref[...] = product[:half]
    other_ref[...] = product[half:]


def combined(parts, weight, layer):
    spec = pl.BlockSpec(memory_space=pltpu.VMEM)
    count, width = parts[0].shape[1], weight.shape[2]
    half = jax.ShapeDtypeStruct((count // CORES, width), BF16)
    return pl.pallas_call(
        functools.partial(combine_kernel, layer=layer),
        out_shape=[half] * 2,
        in_specs=[spec] * len(parts) + [pl.BlockSpec(memory_space=pl.ANY)],
        out_specs=[spec] * 2,
        scratch_shapes=[pltpu.VMEM((HD, width), BF16), pltpu.SemaphoreType.DMA],
        compiler_params=pltpu.CompilerParams(vmem_limit_bytes=8 << 20),
        cost_estimate=pl.CostEstimate(
            flops=2 * count * HD * width, bytes_accessed=2 * HD * width, transcendentals=0
        ),
    )(*parts, weight)


def dot(a, b):
    return jnp.dot(a, b, preferred_element_type=F32).astype(BF16)


def true_rows(count):
    chips = lax.axis_size("chip")
    rows = count // (chips * CORES)
    i = lax.iota(jnp.int32, count)
    block, row = i // rows, i % rows
    core = lax.axis_index("core") ^ (block // chips)
    chip = (lax.axis_index("chip") - block % chips + chips) % chips
    return (chip * CORES + core) * rows + row


def whole(
    source,
    target,
    source_gain,
    attend_gain,
    query_weight,
    key_weight,
    value_weight,
    out_weight,
    mixer_gain,
    gate_weight,
    up_weight,
    gate_taps,
    up_taps,
    down_weight,
    final_gain,
):
    own = normed_rows(source, source_gain).astype(BF16)
    half = own.shape[0] // 2
    behind = block_shift(own, SPAN)
    ahead = block_shift(own, -SPAN)
    far = jnp.concatenate(
        [block_shift(behind[:half], SPAN), block_shift(ahead[half:], -SPAN)],
        axis=0,
    )
    slabs = {"own": own, "side": jnp.concatenate([behind, ahead], axis=0), "far": far}
    pieces = {}
    for name, slab in slabs.items():
        near = from_chips_both_ways(slab) if name == "side" else from_chips(slab)
        pieces[name] = (near, core_swap(near))

    residual = target.astype(F32)
    for layer in range(2):
        normed = normed_rows(residual, attend_gain[layer]).astype(BF16)
        rows = gathered(normed)
        query = dot(rows, query_weight[layer]) * BF16(HD**-0.5)
        if layer == 0:
            own_kv = [project(pieces["own"], key_weight, value_weight, (k,)) for k in range(2)]
            others = [
                project(pieces[name], key_weight, value_weight, (0,))
                for name in ("side", "far")
            ]
        else:
            others = [project(pieces["side"] + pieces["far"], key_weight, value_weight, (layer,))]
        keys, values = zip(own_kv[layer], *others)
        slots = (0,) * len(keys)
        offsets = (1, -1, -2)
        queries = [query] + [block_shift(query, k) for k in offsets]
        parts = attend(queries, keys, values, slots)
        parts = [parts[0]] + [block_shift(part, -k) for part, k in zip(parts[1:], offsets)]
        mine, other = combined(parts, out_weight, layer)
        residual = residual + summed_home(mine, other)

    mixed = gathered(normed_rows(residual, mixer_gain).astype(BF16))
    gated = dot(mixed, gate_weight)
    upped = dot(mixed, up_weight)
    lifted = jnp.concatenate([gated, upped], axis=1)
    count = lifted.shape[0]
    place = lax.optimization_barrier(true_rows(count))
    pad = 8
    edge = lax.iota(jnp.int32, pad)
    pick = jnp.where(edge < HALO, count - HALO + edge, -1)
    last = jnp.dot((pick[:, None] == place[None, :]).astype(BF16), lifted, preferred_element_type=F32)
    earlier = next_block(last.astype(BF16))
    columns = jnp.concatenate([place, jnp.where(edge < HALO, edge - HALO, -count)])
    lifted = jnp.concatenate([lifted, earlier], axis=0)
    taps = jnp.concatenate([gate_taps, up_taps], axis=1)
    convolved = taps[2] * lifted[:count].astype(F32)
    wanted = jnp.concatenate([place - HALO + k for k in range(HALO)])
    moved = jnp.dot(
        (wanted[:, None] == columns[None, :]).astype(BF16), lifted, preferred_element_type=F32
    )
    for k in range(HALO):
        convolved = convolved + taps[k] * moved[k * count : (k + 1) * count]
    inner = gate_weight.shape[1]
    hidden = (jax.nn.silu(convolved[:, :inner]) * convolved[:, inner:]).astype(BF16)
    product = dot(hidden, down_weight)
    half = product.shape[0] // CORES
    residual = residual + summed_home(product[:half], product[half:])
    return normed_rows(residual, final_gain).astype(BF16)


def solution(mesh):
    groups, blocks, _ = mesh.devices.shape
    mesh = Mesh(mesh.devices.reshape(groups, blocks, -1, CORES), ("grp", "sp", *TP))
    placed = (
        P(("grp", "sp", *TP), None),
        P(("grp", "sp", *TP), None),
        P(),
        P(),
        P(None, None, TP),
        P(None, None, TP),
        P(None, None, TP),
        P(None, TP, None),
        P(),
        P(None, TP),
        P(None, TP),
        P(None, TP),
        P(None, TP),
        P(TP, None),
        P(),
    )
    return jax.shard_map(
        whole, mesh=mesh, in_specs=placed, out_specs=P(("grp", "sp", *TP), None), check_vma=False
    )
```

```python
import functools

import jax
import jax.numpy as jnp
from jax import lax
from jax.experimental import pallas as pl
from jax.experimental.pallas import tpu as pltpu
from jax.sharding import Mesh
from jax.sharding import PartitionSpec as P


HD = 256
EPS = 1e-06
CORES = 2
TP = ("chip", "core")
SPAN = 4
STAT_ROWS = 8
HALO = 2
COPY_ROWS = 32
BF16 = jnp.bfloat16
F32 = jnp.float32


def core_swap(value):
    return lax.ppermute(value, "core", [(d, d ^ 1) for d in range(CORES)])


def chip_shift(value, steps):
    count = lax.axis_size("chip")
    return lax.ppermute(value, "chip", [(d, (d + steps) % count) for d in range(count)])


def block_shift(value, steps):
    count = lax.axis_size("sp")
    return lax.ppermute(value, "sp", [(d, (d + steps) % count) for d in range(count)])


def next_block(value):
    count = lax.axis_size("sp")
    return lax.ppermute(value, "sp", [(d, d + 1) for d in range(count - 1)])


def from_chips(rows):
    chips = lax.axis_size("chip")
    return jnp.concatenate([rows] + [chip_shift(rows, k) for k in range(1, chips)], axis=0)


def from_chips_both_ways(rows):
    half = rows.shape[0] // 2
    left = chip_shift(rows, 1)
    right = chip_shift(rows, -1)
    left_far = chip_shift(left[:half], 1)
    right_far = chip_shift(right[half:], -1)
    return jnp.concatenate([rows, left, left_far, right_far, right], axis=0)


def gathered(rows):
    near = from_chips(rows)
    return jnp.concatenate([near, core_swap(near)], axis=0)


def summed_home(mine, other):
    chips = lax.axis_size("chip")
    rows = mine.shape[0] // chips
    mine = mine.astype(F32) + core_swap(other).astype(F32)
    away = mine.astype(BF16)
    total = mine[:rows]
    for k in range(1, chips):
        total = total + chip_shift(away[k * rows : (k + 1) * rows], -k).astype(F32)
    return total


def normed_rows(rows, gain):
    wide = rows.astype(F32)
    return wide * lax.rsqrt(jnp.mean(wide * wide, axis=-1, keepdims=True) + EPS) * gain


def project_kernel(*refs, layers):
    *halves, key_weight_ref, value_weight_ref, key_ref, value_ref, rows_ref = refs
    step = 256
    start = 0
    for ref in halves:

        def copy(i, _, start=start, ref=ref):
            here = pl.ds(pl.multiple_of(i * COPY_ROWS, COPY_ROWS), COPY_ROWS)
            there = pl.ds(pl.multiple_of(start + i * COPY_ROWS, COPY_ROWS), COPY_ROWS)
            rows_ref[there, :] = ref[here, :]
            return 0

        lax.fori_loop(0, ref.shape[0] // COPY_ROWS, copy, 0)
        start += ref.shape[0]
    steps = start // step

    def chunk(i, _):
        here = pl.ds(pl.multiple_of(i % steps * step, step), step)
        slot = i // steps
        layer = layers[0] + slot
        block = rows_ref[here, :]
        keys = jnp.dot(block, key_weight_ref[layer], preferred_element_type=F32)
        key_ref[slot, here, :] = keys.astype(BF16)
        values = jnp.dot(block, value_weight_ref[layer], preferred_element_type=F32)
        value_ref[slot, :, here] = values.T.astype(BF16)
        return 0

    lax.fori_loop(0, len(layers) * steps, chunk, 0)


def project(halves, key_weight, value_weight, layers):
    rows = sum(half.shape[0] for half in halves)
    width = halves[0].shape[1]
    spec = pl.BlockSpec(memory_space=pltpu.VMEM)
    return pl.pallas_call(
        functools.partial(project_kernel, layers=layers),
        out_shape=[
            jax.ShapeDtypeStruct((len(layers), rows, HD), BF16),
            jax.ShapeDtypeStruct((len(layers), HD, rows), BF16),
        ],
        in_specs=[spec] * (len(halves) + 2),
        out_specs=[spec] * 2,
        scratch_shapes=[pltpu.VMEM((rows, width), BF16)],
        compiler_params=pltpu.CompilerParams(vmem_limit_bytes=(6 << 20) + 7 * rows * width),
        cost_estimate=pl.CostEstimate(
            flops=4 * rows * width * HD * len(layers), bytes_accessed=2 * rows * width, transcendentals=0
        ),
    )(*halves, key_weight, value_weight)


def attend_kernel(*refs, pieces, blocks, slots):
    query_refs = refs[:blocks]
    key_refs = refs[blocks : blocks + pieces]
    value_refs = refs[blocks + pieces : blocks + 2 * pieces]
    out_refs = refs[blocks + 2 * pieces : 2 * blocks + 2 * pieces]
    query_all, key_all, value_all, score_ref, summed_ref, out_all = refs[-6:]
    count = query_refs[0].shape[0]
    for k, query_ref in enumerate(query_refs):
        query_all[k * count : (k + 1) * count, :] = query_ref[...]
    start = 0
    for key_ref, value_ref, slot in zip(key_refs, value_refs, slots):
        size = key_ref.shape[1]

        def copy_keys(i, _, start=start, key_ref=key_ref, slot=slot):
            here = pl.ds(pl.multiple_of(i * COPY_ROWS, COPY_ROWS), COPY_ROWS)
            there = pl.ds(pl.multiple_of(start + i * COPY_ROWS, COPY_ROWS), COPY_ROWS)
            key_all[there, :] = key_ref[slot, here, :]
            return 0

        def copy_values(i, _, start=start, size=size, value_ref=value_ref, slot=slot):
            here = pl.ds(pl.multiple_of(i * COPY_ROWS, COPY_ROWS), COPY_ROWS)
            value_all[here, start : start + size] = value_ref[slot, here, :]
            return 0

        lax.fori_loop(0, size // COPY_ROWS, copy_keys, 0)
        lax.fori_loop(0, HD // COPY_ROWS, copy_values, 0)
        start += size
    step = 512
    steps = start // step

    def pair_step(pair, _):
        query = query_all[pl.ds(pl.multiple_of(pair * 2 * count, 2 * count), 2 * count), :]

        def score_step(i, top):
            here = pl.ds(pl.multiple_of(i * step, step), step)
            scores = lax.dot_general(
                key_all[here, :], query, (((1,), (1,)), ((), ())), preferred_element_type=F32
            )
            score_ref[here, :] = scores
            return jnp.maximum(top, jnp.max(scores, axis=0, keepdims=True))

        top = lax.fori_loop(0, steps, score_step, jnp.full((1, 2 * count), -jnp.inf, F32))
        summed_ref[...] = jnp.zeros_like(summed_ref)

        def sum_step(i, total):
            here = pl.ds(pl.multiple_of(i * step, step), step)
            raised = jnp.exp(score_ref[here, :] - top)
            summed_ref[...] += jnp.dot(
                value_all[:, here], raised.astype(BF16), preferred_element_type=F32
            )
            return total + jnp.sum(raised, axis=0, keepdims=True)

        total = lax.fori_loop(0, steps, sum_step, jnp.zeros((1, 2 * count), F32))
        summed = summed_ref[...]
        partial = (summed / total).astype(BF16)
        level = top + jnp.log(total)
        first = level.astype(BF16)
        rest = level - first.astype(F32)
        second = rest.astype(BF16)
        third = (rest - second.astype(F32)).astype(BF16)
        place = lax.broadcasted_iota(jnp.int32, (STAT_ROWS, 2 * count), 0)
        stats = jnp.where(
            place == 0,
            first.astype(F32),
            jnp.where(place == 1, second.astype(F32), jnp.where(place == 2, third.astype(F32), 0.0)),
        ).astype(BF16)
        out_all[pair, :HD, :] = partial
        out_all[pair, HD:, :] = stats
        return 0

    lax.fori_loop(0, blocks // 2, pair_step, 0)
    for k, out_ref in enumerate(out_refs):
        out_ref[...] = out_all[k // 2, :, (k % 2) * count : (k % 2 + 1) * count]


def attend(queries, keys, values, slots):
    count = queries[0].shape[0]
    blocks = len(queries)
    total = sum(k.shape[1] for k in keys)
    spec = pl.BlockSpec(memory_space=pltpu.VMEM)
    return pl.pallas_call(
        functools.partial(attend_kernel, pieces=len(keys), blocks=blocks, slots=slots),
        out_shape=[jax.ShapeDtypeStruct((HD + STAT_ROWS, count), BF16)] * blocks,
        in_specs=[spec] * (blocks + len(keys) + len(values)),
        out_specs=[spec] * blocks,
        scratch_shapes=[
            pltpu.VMEM((blocks * count, HD), BF16),
            pltpu.VMEM((total, HD), BF16),
            pltpu.VMEM((HD, total), BF16),
            pltpu.VMEM((total, 2 * count), F32),
            pltpu.VMEM((HD, 2 * count), F32),
            pltpu.VMEM((blocks // 2, HD + STAT_ROWS, 2 * count), BF16),
        ],
        compiler_params=pltpu.CompilerParams(vmem_limit_bytes=12 << 20),
        cost_estimate=pl.CostEstimate(
            flops=4 * total * count * blocks * HD,
            bytes_accessed=4 * total * HD,
            transcendentals=total * count * blocks,
        ),
    )(*queries, *keys, *values)


def combine_kernel(*refs, layer):
    parts, weight_hbm, mine_ref, other_ref, weight_ref, arrived = refs[:-5], *refs[-5:]
    fetch = pltpu.make_async_copy(weight_hbm.at[layer], weight_ref, arrived)
    fetch.start()
    levels = []
    for part in parts:
        stats = part[HD:, :].astype(F32)
        levels.append(stats[0:1] + stats[1:2] + stats[2:3])
    top = functools.reduce(jnp.maximum, levels)
    shares = [jnp.exp(level - top) for level in levels]
    whole = functools.reduce(jnp.add, shares)
    summed = functools.reduce(
        jnp.add, [part[:HD, :].astype(F32) * (share / whole) for part, share in zip(parts, shares)]
    )
    attended = summed.T.astype(BF16)
    fetch.wait()
    half = mine_ref.shape[0]
    product = jnp.dot(attended, weight_ref[...], preferred_element_type=F32).astype(BF16)
    mine_ref[...] = product[:half]
    other_ref[...] = product[half:]


def combined(parts, weight, layer):
    spec = pl.BlockSpec(memory_space=pltpu.VMEM)
    count, width = parts[0].shape[1], weight.shape[2]
    half = jax.ShapeDtypeStruct((count // CORES, width), BF16)
    return pl.pallas_call(
        functools.partial(combine_kernel, layer=layer),
        out_shape=[half] * 2,
        in_specs=[spec] * len(parts) + [pl.BlockSpec(memory_space=pl.ANY)],
        out_specs=[spec] * 2,
        scratch_shapes=[pltpu.VMEM((HD, width), BF16), pltpu.SemaphoreType.DMA],
        compiler_params=pltpu.CompilerParams(vmem_limit_bytes=8 << 20),
        cost_estimate=pl.CostEstimate(
            flops=2 * count * HD * width, bytes_accessed=2 * HD * width, transcendentals=0
        ),
    )(*parts, weight)


def dot(a, b):
    return jnp.dot(a, b, preferred_element_type=F32).astype(BF16)


def true_rows(count):
    chips = lax.axis_size("chip")
    rows = count // (chips * CORES)
    i = lax.iota(jnp.int32, count)
    block, row = i // rows, i % rows
    core = lax.axis_index("core") ^ (block // chips)
    chip = (lax.axis_index("chip") - block % chips + chips) % chips
    return (chip * CORES + core) * rows + row


def whole(
    source,
    target,
    source_gain,
    attend_gain,
    query_weight,
    key_weight,
    value_weight,
    out_weight,
    mixer_gain,
    gate_weight,
    up_weight,
    gate_taps,
    up_taps,
    down_weight,
    final_gain,
):
    own = normed_rows(source, source_gain).astype(BF16)
    half = own.shape[0] // 2
    behind = block_shift(own, SPAN)
    ahead = block_shift(own, -SPAN)
    far = jnp.concatenate(
        [block_shift(behind[:half], SPAN), block_shift(ahead[half:], -SPAN)],
        axis=0,
    )
    slabs = {"own": own, "side": jnp.concatenate([behind, ahead], axis=0), "far": far}
    pieces = {}
    for name, slab in slabs.items():
        near = from_chips_both_ways(slab) if name == "side" else from_chips(slab)
        pieces[name] = (near, core_swap(near))

    residual = target.astype(F32)
    for layer in range(2):
        normed = normed_rows(residual, attend_gain[layer]).astype(BF16)
        rows = gathered(normed)
        query = dot(rows, query_weight[layer]) * BF16(HD**-0.5)
        if layer == 0:
            own_kv = [project(pieces["own"], key_weight, value_weight, (k,)) for k in range(2)]
            others = [
                project(pieces[name], key_weight, value_weight, (0,))
                for name in ("side", "far")
            ]
        else:
            others = [
                project(pieces[name], key_weight, value_weight, (layer,))
                for name in ("side", "far")
            ]
        keys, values = zip(own_kv[layer], *others)
        slots = (0,) * len(keys)
        offsets = (1, -1, -2)
        queries = [query] + [block_shift(query, k) for k in offsets]
        parts = attend(queries, keys, values, slots)
        parts = [parts[0]] + [block_shift(part, -k) for part, k in zip(parts[1:], offsets)]
        mine, other = combined(parts, out_weight, layer)
        residual = residual + summed_home(mine, other)

    mixed = gathered(normed_rows(residual, mixer_gain).astype(BF16))
    gated = dot(mixed, gate_weight)
    upped = dot(mixed, up_weight)
    lifted = jnp.concatenate([gated, upped], axis=1)
    count = lifted.shape[0]
    place = lax.optimization_barrier(true_rows(count))
    pad = 8
    edge = lax.iota(jnp.int32, pad)
    pick = jnp.where(edge < HALO, count - HALO + edge, -1)
    last = jnp.dot((pick[:, None] == place[None, :]).astype(BF16), lifted, preferred_element_type=F32)
    earlier = next_block(last.astype(BF16))
    columns = jnp.concatenate([place, jnp.where(edge < HALO, edge - HALO, -count)])
    lifted = jnp.concatenate([lifted, earlier], axis=0)
    taps = jnp.concatenate([gate_taps, up_taps], axis=1)
    convolved = taps[2] * lifted[:count].astype(F32)
    wanted = jnp.concatenate([place - HALO + k for k in range(HALO)])
    moved = jnp.dot(
        (wanted[:, None] == columns[None, :]).astype(BF16), lifted, preferred_element_type=F32
    )
    for k in range(HALO):
        convolved = convolved + taps[k] * moved[k * count : (k + 1) * count]
    inner = gate_weight.shape[1]
    hidden = (jax.nn.silu(convolved[:, :inner]) * convolved[:, inner:]).astype(BF16)
    product = dot(hidden, down_weight)
    half = product.shape[0] // CORES
    residual = residual + summed_home(product[:half], product[half:])
    return normed_rows(residual, final_gain).astype(BF16)


def solution(mesh):
    groups, blocks, _ = mesh.devices.shape
    mesh = Mesh(mesh.devices.reshape(groups, blocks, -1, CORES), ("grp", "sp", *TP))
    placed = (
        P(("grp", "sp", *TP), None),
        P(("grp", "sp", *TP), None),
        P(),
        P(),
        P(None, None, TP),
        P(None, None, TP),
        P(None, None, TP),
        P(None, TP, None),
        P(),
        P(None, TP),
        P(None, TP),
        P(None, TP),
        P(None, TP),
        P(TP, None),
        P(),
    )
    return jax.shard_map(
        whole, mesh=mesh, in_specs=placed, out_specs=P(("grp", "sp", *TP), None), check_vma=False
    )
```
